32 devices in a mesh: fs: 16 (over z, y, x), tp: 2 (over core).
Axes of the slice: x: 2, y: 2, z: 4, core: 2. Of those that a mesh axis runs over, the one named last changes fastest.
Arguments:
- tokens: bfloat16 [2, 256, 2048], P('tp'), may hold values from -6 to 6
- gain_first: float32 [2048], P('fs'), may hold values from 0.1 to 1.9
- gate_first: float32 [2048, 5632], P('fs', 'tp'), may hold values from -0.125 to 0.125
- up_first: float32 [2048, 5632], P('fs', 'tp'), may hold values from -0.125 to 0.125
- down_first: float32 [2048, 5632], P('fs', 'tp'), may hold values from -0.3125 to 0.3125
- gain_second: float32 [2048], P('fs'), may hold values from 0.1 to 1.9
- gate_second: float32 [2048, 5632], P('fs', 'tp'), may hold values from -0.125 to 0.125
- up_second: float32 [2048, 5632], P('fs', 'tp'), may hold values from -0.125 to 0.125
- down_second: float32 [2048, 5632], P('fs', 'tp'), may hold values from -0.3125 to 0.3125
Outputs:
- mixed: bfloat16 [2, 256, 2048], P('tp', 'fs')
- served_gate_first: bfloat16 [2, 2816, 2048], P(None, 'fs')
- served_up_first: bfloat16 [2, 2816, 2048], P(None, 'fs')
- served_down_first: bfloat16 [2, 2816, 2048], P(None, 'fs')
- served_gate_second: bfloat16 [2, 2816, 2048], P(None, 'fs')
- served_up_second: bfloat16 [2, 2816, 2048], P(None, 'fs')
- served_down_second: bfloat16 [2, 2816, 2048], P(None, 'fs')
The draws below stay inside these ranges and needn't reach their ends.
All inputs are finite; a program needn't handle non-finite values.
Results may differ from the reference program's by a relative error of at most 0.013.
Values may be sent and summed in bfloat16 or wider, within the bound.
No kernel may reach another device: no remote copies, remote signals or barrier semaphores. Data moves between devices by JAX's collectives and lax.ppermute only.
A program may use at most 64 MiB of HBM per device.

```python
import jax
import jax.numpy as jnp
from jax import lax

D = 2048
FF = 5632
PLEN = 256
PROMPTS = 2
N_TP = 2


def steps_of(key, dims, pieces, smallest, largest):
    loudness = 1.0
    for position, blocks in pieces:
        draws = jax.random.uniform(jax.random.fold_in(jax.random.fold_in(key, 6), position), (blocks,), jnp.float32, smallest / len(pieces), largest / len(pieces))
        loudness = loudness * jnp.repeat(jnp.exp(draws), dims[position] // blocks).reshape((-1,) + (1,) * (len(dims) - 1 - position))
    return loudness


def bell_draw(rng, dims, width, reach, split=(), kind=jnp.bfloat16):
    values = jax.random.normal(rng, dims, jnp.float32) * width
    if len(split) > 0:
        values = steps_of(rng, dims, split, -0.22, 0.18) * values
    return jnp.clip(values, min=-reach, max=reach).astype(kind)


def setup_inputs(seed: int = 0) -> dict:
    keys = jax.random.split(jax.random.key(seed), 10)
    tokens = bell_draw(keys[0], (PROMPTS, PLEN, D), 1.0, 6.0, ((0, 2),))
    gain_first = jnp.clip(1.0 + 0.18 * jax.random.normal(keys[1], (D,), jnp.float32), 0.1, 1.9)
    gate_first = bell_draw(keys[2], (D, FF), D ** -0.5, 0.125, ((0, 16), (1, 2)), jnp.float32)
    up_first = bell_draw(keys[3], (D, FF), D ** -0.5, 0.125, ((0, 16), (1, 2)), jnp.float32)
    down_first = bell_draw(keys[4], (D, FF), (FF // 16) ** -0.5, 0.3125, ((0, 16), (1, 2)), jnp.float32)
    gain_second = jnp.clip(1.0 + 0.18 * jax.random.normal(keys[5], (D,), jnp.float32), 0.1, 1.9)
    gate_second = bell_draw(keys[6], (D, FF), D ** -0.5, 0.125, ((0, 16), (1, 2)), jnp.float32)
    up_second = bell_draw(keys[7], (D, FF), D ** -0.5, 0.125, ((0, 16), (1, 2)), jnp.float32)
    down_second = bell_draw(keys[8], (D, FF), (FF // 16) ** -0.5, 0.3125, ((0, 16), (1, 2)), jnp.float32)
    return {"tokens": tokens, "gain_first": gain_first, "gate_first": gate_first, "up_first": up_first, "down_first": down_first, "gain_second": gain_second, "gate_second": gate_second, "up_second": up_second, "down_second": down_second}


def normalize(values):
    wide = values.astype(jnp.float32)
    scale = lax.rsqrt(lax.optimization_barrier(jnp.mean(wide * wide, axis=-1, keepdims=True)) + 1e-06)
    return (wide * scale).astype(jnp.bfloat16)

def gated_branch(values, gate_cast, up_cast, down_cast):
    normed = normalize(values)
    gate_act = jnp.dot(normed, gate_cast, preferred_element_type=jnp.float32)
    up_act = jnp.dot(normed, up_cast, preferred_element_type=jnp.float32)
    hidden = (jax.nn.silu(gate_act) * up_act).astype(jnp.bfloat16)
    return jnp.dot(hidden, down_cast.T, preferred_element_type=jnp.float32)

def served(cast):
    return cast.T.reshape(N_TP, FF // N_TP, D)

def reference(tokens, gain_first, gate_first, up_first, down_first, gain_second, gate_second, up_second, down_second):
    gate_one = (gate_first * gain_first[:, None]).astype(jnp.bfloat16)
    up_one = (up_first * gain_first[:, None]).astype(jnp.bfloat16)
    down_one = down_first.astype(jnp.bfloat16)
    gate_two = (gate_second * gain_second[:, None]).astype(jnp.bfloat16)
    up_two = (up_second * gain_second[:, None]).astype(jnp.bfloat16)
    down_two = down_second.astype(jnp.bfloat16)
    rows = tokens.reshape(-1, D)
    branch_first = gated_branch(rows, gate_one, up_one, down_one)
    middle = (rows.astype(jnp.float32) + 0.5 * branch_first).astype(jnp.bfloat16)
    branch_second = gated_branch(middle, gate_two, up_two, down_two)
    mixed = (middle.astype(jnp.float32) + 0.5 * branch_second).astype(jnp.bfloat16)
    return (mixed.reshape(tokens.shape), served(gate_one), served(up_one), served(down_one), served(gate_two), served(up_two), served(down_two))
```

```python
import functools

import jax
import jax.numpy as jnp
from jax import lax
from jax.experimental import pallas as pl
from jax.experimental.pallas import tpu as pltpu
from jax.sharding import PartitionSpec as P


LANES = 128
PACK = 16


def normalize(values):
    wide = values.astype(jnp.float32)
    scale = lax.rsqrt(jnp.mean(wide * wide, axis=-1, keepdims=True) + 1e-06)
    return (wide * scale).astype(jnp.bfloat16)


def folded(weight, gain):
    return (weight * gain[:, None]).astype(jnp.bfloat16).T


def hidden_of(normed, gate_served, up_served):
    gate_flat = gate_served.reshape(-1, gate_served.shape[2])
    up_flat = up_served.reshape(-1, up_served.shape[2])
    gate_act = jnp.einsum("rd,hd->rh", normed, gate_flat, preferred_element_type=jnp.float32)
    up_act = jnp.einsum("rd,hd->rh", normed, up_flat, preferred_element_type=jnp.float32)
    return (jax.nn.silu(gate_act) * up_act).astype(jnp.bfloat16)


def partial_branch(normed, gate_served, up_served, down_served):
    hidden = hidden_of(normed, gate_served, up_served)
    down_flat = down_served.reshape(-1, down_served.shape[2])
    return jnp.dot(hidden, down_flat, preferred_element_type=jnp.float32)


def swap(values, size, bits):
    return lax.ppermute(values, "fs", [(i, i ^ bits) for i in range(size)])


def offsets_of(size):
    return [low | (high << 2) for low in range(4) for high in range(size // 4)]


def reduce_to_mine(partial, size):
    for members, shift in ((4, 0), (size // 4, 2)):
        parts = partial.reshape(members, -1, partial.shape[1])
        arrived = [swap(parts[m].astype(jnp.bfloat16), size, m << shift) for m in range(1, members)]
        partial = parts[0]
        for part in arrived:
            partial = partial + part.astype(jnp.float32)
    return partial


def gather_all(rows, size):
    for members, shift in ((size // 4, 2), (4, 0)):
        rows = jnp.concatenate([rows] + [swap(rows, size, m << shift) for m in range(1, members)], axis=0)
    return rows


def unpack(own, other):
    size, count, rows, lanes = own.shape
    step = 4

    def kernel(own_ref, other_ref, *out_refs):
        mine = lax.axis_index("tp")
        for j in range(step):
            columns = slice(j * lanes, (j + 1) * lanes)
            for w in range(count):
                out_refs[w][mine, :, columns] = own_ref[j, w]
                out_refs[w][1 - mine, :, columns] = other_ref[j, w]

    block = pl.BlockSpec((step, count, rows, lanes), lambda i: (i, 0, 0, 0))
    out = pl.BlockSpec((2, rows, step * lanes), lambda i: (0, 0, i))
    shape = jax.ShapeDtypeStruct((2, rows, size * lanes), own.dtype)
    return pl.pallas_call(
        kernel,
        grid=(size // step,),
        in_specs=[block, block],
        out_specs=[out] * count,
        out_shape=[shape] * count,
        cost_estimate=pl.CostEstimate(flops=6_000_000, bytes_accessed=4 * own.size * 2, transcendentals=0),
        name="unpack",
    )(own, other)


def packed(gate, up, down, gain, size):
    parts = [folded(gate, gain), folded(up, gain), down.astype(jnp.bfloat16).T]
    parts = [part.reshape(size, -1, part.shape[1]) for part in parts]
    return jnp.stack(parts, axis=1)


def tp_swap(values):
    return lax.ppermute(values, "tp", [(0, 1), (1, 0)])


def fast_shards(
    tokens,
    gain_first,
    gate_first,
    up_first,
    down_first,
    gain_second,
    gate_second,
    up_second,
    down_second,
):
    size = lax.axis_size("fs")
    me = lax.axis_index("fs")
    rows = tokens[0]
    keep = rows.shape[0] // size
    turned = jnp.take(rows.reshape(size, keep, -1), me ^ jnp.array(offsets_of(size)), axis=0)
    mine = turned[0]
    normed_first = normalize(turned.reshape(rows.shape))

    first = packed(gate_first, up_first, down_first, gain_first, size)
    second = packed(gate_second, up_second, down_second, gain_second, size)
    first = lax.all_to_all(first, "fs", split_axis=0, concat_axis=0, tiled=True)
    first, second = lax.optimization_barrier((first, second))
    second = lax.all_to_all(second, "fs", split_axis=0, concat_axis=0, tiled=True)
    gate_one, up_one, down_one = unpack(first, tp_swap(first))
    gate_two, up_two, down_two = unpack(second, tp_swap(second))

    branch = reduce_to_mine(partial_branch(normed_first, gate_one, up_one, down_one), size)
    middle = (mine.astype(jnp.float32) + 0.5 * branch).astype(jnp.bfloat16)
    normed_second = gather_all(normalize(middle), size)
    branch_two = reduce_to_mine(partial_branch(normed_second, gate_two, up_two, down_two), size)
    mixed = (middle.astype(jnp.float32) + 0.5 * branch_two).astype(jnp.bfloat16)[None]
    return (mixed, gate_one, up_one, down_one, gate_two, up_two, down_two)


def relayout(*parts):
    cuts = [lax.all_to_all(part, "fs", split_axis=0, concat_axis=1, tiled=True) for part in parts]
    return [lax.all_gather(cut[None], "tp", axis=0, tiled=True) for cut in cuts]


def plain_shards(
    tokens,
    gain_first,
    gate_first,
    up_first,
    down_first,
    gain_second,
    gate_second,
    up_second,
    down_second,
):
    gate_one, up_one, down_one = relayout(
        folded(gate_first, gain_first),
        folded(up_first, gain_first),
        down_first.astype(jnp.bfloat16).T,
    )
    gate_two, up_two, down_two = relayout(
        folded(gate_second, gain_second),
        folded(up_second, gain_second),
        down_second.astype(jnp.bfloat16).T,
    )
    rows = tokens[0]
    keep = rows.shape[0] // lax.axis_size("fs")
    offset = lax.axis_index("fs") * keep
    branch = lax.psum(partial_branch(normalize(rows), gate_one, up_one, down_one), "fs")
    whole_middle = (rows.astype(jnp.float32) + 0.5 * branch).astype(jnp.bfloat16)
    middle = lax.dynamic_slice_in_dim(whole_middle, offset, keep, 0)
    branch_two = lax.psum_scatter(
        partial_branch(normalize(whole_middle), gate_two, up_two, down_two), "fs", scatter_dimension=0, tiled=True
    )
    mixed = (middle.astype(jnp.float32) + 0.5 * branch_two).astype(jnp.bfloat16)[None]
    return (mixed, gate_one, up_one, down_one, gate_two, up_two, down_two)


def solution(mesh):
    fs, tp = mesh.shape["fs"], mesh.shape["tp"]

    def shards(tokens, gain_first, gate_first, *others):
        features, units = gate_first.shape
        fits = (
            tp == 2
            and fs >= 16
            and fs & (fs - 1) == 0
            and features % LANES == 0
            and units % (fs * PACK) == 0
            and tokens.shape[0] == 1
            and tokens.shape[1] % (fs * PACK) == 0
        )
        run = fast_shards if fits else plain_shards
        return run(tokens, gain_first, gate_first, *others)

    return jax.shard_map(
        shards,
        mesh=mesh,
        in_specs=(
            P("tp", None, None),
            P("fs"),
            P("fs", "tp"),
            P("fs", "tp"),
            P("fs", "tp"),
            P("fs"),
            P("fs", "tp"),
            P("fs", "tp"),
            P("fs", "tp"),
        ),
        out_specs=(
            P("tp", "fs", None),
            P(None, "fs", None),
            P(None, "fs", None),
            P(None, "fs", None),
            P(None, "fs", None),
            P(None, "fs", None),
            P(None, "fs", None),
        ),
        check_vma=False,
    )
```
